32 devices in a mesh: sp: 8 (over z, x), tp: 4 (over y, core).
Axes of the slice: x: 2, y: 2, z: 4, core: 2. Of those that a mesh axis runs over, the one named last changes fastest.
Arguments:
- mixed: bfloat16 [1024, 2048], P('sp'), may hold values from -6 to 6
- cotangent: bfloat16 [1024, 2048], P('sp'), may hold values from -6 to 6
- routes: int32 [1024, 2], P('sp'), may hold values from 0 to 7, all different within a row; in each aligned block of 128 rows (0 to 127, 128 to 255, ...) at most 64 rows name the same one
- gates: float32 [1024, 2], P('sp'), may hold values from 0.1 to 1
- w_gate: bfloat16 [8, 2048, 1024], P('sp', None, 'tp'), may hold values from -0.125 to 0.125
- w_up: bfloat16 [8, 2048, 1024], P('sp', None, 'tp'), may hold values from -0.125 to 0.125
- w_down: bfloat16 [8, 1024, 2048], P('sp', 'tp'), may hold values from -0.1875 to 0.1875
- out_weight: bfloat16 [1024, 2048], P('tp'), may hold values from -0.1875 to 0.1875
- gate_pre: bfloat16 [1024, 1024], P('sp', 'tp'), may hold values from -8 to 8
- mixer_out: bfloat16 [1024, 1024], P('sp', 'tp'), may hold values from -6 to 6
- values: bfloat16 [1024, 1024], P('sp', 'tp'), may hold values from -6 to 6
- write_keys: bfloat16 [1024, 512], P('sp', 'tp'), may hold values from -1.25 to 1.25
- read_keys: bfloat16 [1024, 512], P('sp', 'tp'), may hold values from -1.25 to 1.25
- log_decay: float32 [16, 1024], P('tp', 'sp'), may hold values from -0.08 to 0
- entry_states: float32 [8, 16, 64, 128], P('sp', 'tp'), may hold values from -6 to 6
Outputs:
- d_w_gate: bfloat16 [8, 2048, 1024], P('sp', None, 'tp')
- d_w_up: bfloat16 [8, 2048, 1024], P('sp', None, 'tp')
- d_w_down: bfloat16 [8, 1024, 2048], P('sp', 'tp')
- d_out_weight: float32 [2048, 1024], P('sp', 'tp')
- d_input: bfloat16 [1024, 2048], P('sp', 'tp')
- d_values: bfloat16 [1024, 1024], P('sp', 'tp')
- d_write: float32 [1024, 512], P('sp', 'tp')
- d_read: float32 [1024, 512], P('sp', 'tp')
- d_gate: bfloat16 [1024, 1024], P('sp', 'tp')
The draws below stay inside these ranges and needn't reach their ends.
Inputs may be any that keep to these rules, and one draw needn't show every extreme that they name: `routes`: each row names 2 different experts; in the 128 rows of one device no expert is named more than 64 times, and in some blocks one is named exactly 64 times.
All inputs are finite; a program needn't handle non-finite values.
Results may differ from the reference program's by a relative error of at most 0.0062.
Values may be sent and summed in bfloat16 or wider, within the bound.
A program may use at most 64 MiB of HBM per device.

```python
import math
import jax
import jax.numpy as jnp
import numpy as np
from jax import lax

D = 2048
FF_E = 1024
HEAD_DIM = 64
STATE = 128
HPG = 4
BLOCK = 128
TOPK = 2
TOK_DEV = 128
GROUPS = 4
HEADS = 16
D_INNER = 1024
EXPERTS = 8
TOKENS = 1024
CAP = 64
NBLK = 8
N_SP = 8
N_TP = 4


def draw_log_decay(key, part):
    key_set = jax.random.split(key, 3)
    chooser = jax.random.uniform(key_set[0], (HEADS, 1))
    fast_head = chooser < 0.5
    base_rate = jnp.where(fast_head, 1.0 / 40.0, 0.5 / TOKENS)
    shard_scale = jnp.exp(jax.random.uniform(key_set[1], (HEADS, TOKENS // TOK_DEV), minval=-0.7, maxval=0.7))
    shard_scale = jnp.repeat(shard_scale, TOK_DEV, axis=1)
    jitter = jax.random.uniform(key_set[2], (HEADS, TOKENS), minval=0.5, maxval=1.5)
    return -(base_rate * shard_scale * jitter)


def strengthened(values, own_key, source, target, shards_of, factor):
    owner, partner = [(jnp.arange(values.shape[dim]) // (values.shape[dim] // shards_of)).reshape([-1 if axis == dim else 1 for axis in range(values.ndim)]) for dim in (source, target)]
    chosen = jax.random.permutation(own_key, shards_of)[partner]
    strong = (owner == chosen) | (owner == (partner + shards_of // 2) % shards_of)
    return jnp.where(strong, factor * values, values)


def block_scale(key, shape, shards, smallest, high):
    loudness, own = 1.0, jax.random.fold_in(key, 6)
    for axis_at, parts in shards:
        steps = jnp.exp(jax.random.uniform(jax.random.fold_in(own, axis_at), (parts,), jnp.float32, smallest / len(shards), high / len(shards)))
        loudness = loudness * jnp.repeat(steps, shape[axis_at] // parts).reshape([-1 if axis == axis_at else 1 for axis in range(len(shape))])
    return loudness


def assign_block(stream_key, own, number, rows, count, top, limit, skew):
    sequence = jax.random.permutation(stream_key, count)
    packed, usual = load_shares(count, rows * top, limit, skew, True), load_shares(count, rows * top, limit, skew, False)
    places = jnp.arange(count)

    def named(tallies, turn):
        used = int((tallies > 0).sum())
        fixed = max(1, used // 4)
        passed = fixed + (places - fixed + turn * (used - fixed)) % max(1, count - fixed)
        return jnp.zeros((count,), jnp.int32).at[sequence[jnp.where(places < fixed, places, passed)]].set(jnp.asarray(tallies, jnp.int32))

    tallies = jnp.where(number % 4 == 0, named(packed, number // 4), named(usual, number - number // 4 - 1))
    mixed = jax.random.permutation(jax.random.fold_in(own, 3), count)
    source_of, receiver = mixed[0:count // 2 * 2:2], mixed[1:count // 2 * 2:2]
    slack = jnp.minimum(tallies[source_of] - 1, limit - tallies[receiver]) // 2
    slack = jnp.where((source_of == sequence[0]) | (receiver == sequence[0]) | (tallies[receiver] == 0), 0, jnp.maximum(slack, 0))
    passed = jax.random.randint(jax.random.fold_in(own, 4), (count // 2,), 0, 1 << 20) % (slack + 1)
    tallies = tallies.at[source_of].add(-passed).at[receiver].add(passed)
    members = jnp.searchsorted(jnp.cumsum(tallies), jnp.arange(rows * top), side="right").astype(jnp.int32)
    listing = members.reshape(top, rows).T
    listing = listing[jax.random.permutation(jax.random.fold_in(own, 1), rows)]
    turn = jax.random.randint(jax.random.fold_in(own, 2), (rows, 1), 0, top)
    return jnp.take_along_axis(listing, (jnp.arange(top)[None, :] + turn) % top, axis=1)


def load_shares(count, total, limit, slope, full):
    loads = [(1 << 20) // math.isqrt(grade ** slope) + 1 for grade in range(1, count + 1)]
    largest = limit if full else min(limit, max(-(-total // count), total * loads[0] // sum(loads)))
    least = 1 if total - largest >= count - 1 else 0
    counts, rest = [largest] + [least] * (count - 1), total - largest - least * (count - 1)
    while rest > 0:
        candidates = [i for i in range(1, count) if counts[i] < largest] or [i for i in range(1, count) if counts[i] < limit]
        whole, budget = sum([loads[i] for i in candidates]), rest
        for i in candidates:
            addition = min(limit - counts[i], max(1, budget * loads[i] // whole), rest)
            counts[i] = counts[i] + addition
            rest = rest - addition
    return np.array(counts)


def bell_draw(stream_key, shape, width, reach, shards=(), kind=jnp.bfloat16):
    entries = jax.random.normal(stream_key, shape, jnp.float32) * width
    if len(shards) > 0:
        entries = block_scale(stream_key, shape, shards, -0.22, 0.18) * entries
    return jnp.clip(entries, min=-reach, max=reach).astype(kind)


def noise_with(stream_key, shape, width, reach, shards, heavy, kind=jnp.bfloat16):
    drawn = width * jax.random.normal(stream_key, shape, jnp.float32)
    if shards:
        drawn = drawn * block_scale(stream_key, shape, shards, -0.22, 0.18)
    return jnp.clip(strengthened(drawn, jax.random.fold_in(stream_key, 3), *heavy), -reach, reach).astype(kind)


def setup_inputs(seed: int = 0) -> dict:
    arg_keys = jax.random.split(jax.random.key(seed), 16)
    mixed = bell_draw(arg_keys[0], (TOKENS, D), 1.0, 6.0, ((0, 8),))
    cotangent = noise_with(arg_keys[1], (TOKENS, D), 1.0, 6.0, ((0, 8),), (0, 1, 8, 2.0))
    routes_keys = jax.random.split(jax.random.fold_in(arg_keys[2], 1), TOKENS // TOK_DEV)
    routes_turns = jax.random.permutation(jax.random.fold_in(arg_keys[2], 3), TOKENS // TOK_DEV)
    routes = jax.vmap(lambda own, number: assign_block(jax.random.fold_in(arg_keys[2], 2), own, number, TOK_DEV, EXPERTS, TOPK, CAP, 2))(routes_keys, routes_turns).reshape((TOKENS, TOPK))
    gates = jnp.clip(0.1 + 0.9 * jax.random.uniform(arg_keys[3], (TOKENS, TOPK), jnp.float32) ** block_scale(arg_keys[3], (TOKENS, TOPK), ((0, 8),), -0.2, 0.2), 0.1, 1.0)
    w_gate = bell_draw(arg_keys[4], (EXPERTS, D, FF_E), D ** -0.5, 0.125, ((0, 8), (2, 4)))
    w_up = bell_draw(arg_keys[5], (EXPERTS, D, FF_E), D ** -0.5, 0.125, ((0, 8), (2, 4)))
    w_down = bell_draw(arg_keys[6], (EXPERTS, FF_E, D), FF_E ** -0.5, 0.1875, ((0, 8), (1, 4)))
    out_weight = bell_draw(arg_keys[7], (D_INNER, D), D_INNER ** -0.5, 0.1875, ((0, 4),))
    gate_pre = bell_draw(arg_keys[8], (TOKENS, D_INNER), 1.5, 8.0, ((0, 8), (1, 4)))
    mixer_out = bell_draw(arg_keys[9], (TOKENS, D_INNER), 1.0, 6.0, ((0, 8), (1, 4)))
    values = bell_draw(arg_keys[10], (TOKENS, D_INNER), 1.0, 6.0, ((0, 8), (1, 4)))
    write_keys = bell_draw(arg_keys[11], (TOKENS, GROUPS * STATE), 0.2, 1.25, ((0, 8), (1, 4)))
    read_keys = bell_draw(arg_keys[12], (TOKENS, GROUPS * STATE), 0.2, 1.25, ((0, 8), (1, 4)))
    log_decay = draw_log_decay(jax.random.fold_in(arg_keys[15], 71), 0)
    entry_states = bell_draw(arg_keys[14], (NBLK, HEADS, HEAD_DIM, STATE), 1.0, 6.0, ((0, 8), (1, 4)), jnp.float32)
    return dict(mixed=mixed, cotangent=cotangent, routes=routes, gates=gates, w_gate=w_gate, w_up=w_up, w_down=w_down, out_weight=out_weight, gate_pre=gate_pre, mixer_out=mixer_out, values=values, write_keys=write_keys, read_keys=read_keys, log_decay=log_decay, entry_states=entry_states)


precise = lax.Precision.HIGHEST

def silu_grad(pre_act):
    logistic = jax.nn.sigmoid(pre_act)
    return logistic * (1.0 + pre_act * (1.0 - logistic))

def expert_back(inputs):
    tok_rows, cot_rows, weight_g, weight_u, weight_d = inputs
    pre_gate = jnp.dot(tok_rows, weight_g, preferred_element_type=jnp.float32)
    pre_up = jnp.dot(tok_rows, weight_u, preferred_element_type=jnp.float32)
    active = jax.nn.silu(pre_gate)
    hidden = (active * pre_up).astype(jnp.bfloat16)
    grad_down = jnp.dot(hidden.T, cot_rows, preferred_element_type=jnp.float32)
    grad_hidden = jnp.dot(cot_rows, weight_d.T, preferred_element_type=jnp.float32)
    grad_gate = (grad_hidden * pre_up * silu_grad(pre_gate)).astype(jnp.bfloat16)
    grad_upval = (grad_hidden * active).astype(jnp.bfloat16)
    grad_wg = jnp.dot(tok_rows.T, grad_gate, preferred_element_type=jnp.float32)
    grad_wu = jnp.dot(tok_rows.T, grad_upval, preferred_element_type=jnp.float32)
    part_width = FF_E // N_TP
    gate_parts = grad_gate.astype(jnp.float32).reshape(-1, N_TP, part_width)
    up_parts = grad_upval.astype(jnp.float32).reshape(-1, N_TP, part_width)
    wg_parts = weight_g.astype(jnp.float32).reshape(D, N_TP, part_width)
    wu_parts = weight_u.astype(jnp.float32).reshape(D, N_TP, part_width)
    partial_value = jnp.einsum('rif,dif->ird', gate_parts, wg_parts) + jnp.einsum('rif,dif->ird', up_parts, wu_parts)
    rounded = lax.optimization_barrier(partial_value.astype(jnp.bfloat16))
    summed = lax.optimization_barrier(jnp.sum(rounded.astype(jnp.float32), axis=0))
    return (grad_wg.astype(jnp.bfloat16), grad_wu.astype(jnp.bfloat16), grad_down.astype(jnp.bfloat16), summed.astype(jnp.bfloat16))

def block_back(grad_state, inputs):
    inputs_x, grad_y, log_rate, write_rows, read_rows, start_state = inputs
    block_len = log_rate.shape[0]
    running = jnp.cumsum(log_rate, axis=0)
    causal_mask = (jnp.arange(block_len)[:, None] >= jnp.arange(block_len)[None, :])[:, :, None, None]
    spread = running[:, None] - running[None, :]
    decay_mat = jnp.where(causal_mask, jnp.exp(jnp.where(causal_mask, spread, 0.0)), 0.0)
    intersection = jnp.einsum('lgn,sgn->lsg', read_rows, write_rows, precision=precise)
    mixing = intersection[..., None] * decay_mat
    to_end = jnp.exp(running[-1][None] - running)
    from_start = jnp.exp(running)
    grad_x = jnp.einsum('lsgj,lgjp->sgjp', mixing, grad_y, precision=precise) + to_end[..., None] * jnp.einsum('sgn,gjpn->sgjp', write_rows, grad_state, precision=precise)
    weighted = jnp.einsum('lgjp,sgjp->lsgj', grad_y, inputs_x, precision=precise) * decay_mat
    grad_w = jnp.einsum('lsgj,lgn->sgn', weighted, read_rows, precision=precise) + jnp.einsum('sgj,sgjp,gjpn->sgn', to_end, inputs_x, grad_state, precision=precise)
    grad_r = jnp.einsum('lsgj,sgn->lgn', weighted, write_rows, precision=precise) + jnp.einsum('lgj,lgjp,gjpn->lgn', from_start, grad_y, start_state, precision=precise)
    earlier = jnp.exp(running[-1])[..., None, None] * grad_state + jnp.einsum('lgj,lgjp,lgn->gjpn', from_start, grad_y, read_rows, precision=precise)
    return (earlier, (grad_x, grad_w, grad_r))

def reference(mixed, cotangent, routes, gates, w_gate, w_up, w_down, out_weight, gate_pre, mixer_out, values, write_keys, read_keys, log_decay, entry_states):
    assigned = TOKENS * TOPK
    picks = routes.reshape(N_SP, TOK_DEV * TOPK)
    onehot = (picks[:, :, None] == jnp.arange(EXPERTS, dtype=jnp.int32)[None, None, :]).astype(jnp.int32)
    earlier_same = jnp.cumsum(onehot, axis=1) - onehot
    slot_of = lax.optimization_barrier(jnp.sum(earlier_same * onehot, axis=2))
    shard_ids = jnp.arange(N_SP, dtype=jnp.int32)[:, None]
    target = ((picks * N_SP + shard_ids) * CAP + slot_of).reshape(assigned).astype(jnp.int32)
    anchor = jnp.full((EXPERTS * N_SP * CAP,), assigned, jnp.int32).at[target].set(jnp.arange(assigned, dtype=jnp.int32))
    scaled = (gates[:, :, None] * cotangent[:, None, :].astype(jnp.float32)).astype(jnp.bfloat16).reshape(assigned, D)
    empty_row = jnp.zeros((1, D), jnp.bfloat16)
    cot_rows = jnp.concatenate([scaled, empty_row])[anchor].reshape(EXPERTS, N_SP * CAP, D)
    tok_rows = jnp.concatenate([mixed, empty_row])[anchor // TOPK].reshape(EXPERTS, N_SP * CAP, D)
    grad_wg, grad_wu, grad_down, row_grad = lax.map(expert_back, (tok_rows, cot_rows, w_gate, w_up, w_down))
    picked = row_grad.reshape(EXPERTS * N_SP * CAP, D)[target].reshape(TOKENS, TOPK, D).astype(jnp.float32)
    d_input = (cotangent.astype(jnp.float32) + lax.optimization_barrier(jnp.sum(picked, axis=1))).astype(jnp.bfloat16)
    back_proj = jnp.dot(d_input, out_weight.T, preferred_element_type=jnp.float32)
    pre_act = gate_pre.astype(jnp.float32)
    gate_act = jax.nn.silu(pre_act)
    saved_out = mixer_out.astype(jnp.float32)
    d_gate = (back_proj * saved_out * silu_grad(pre_act)).astype(jnp.bfloat16)
    gated = (saved_out * gate_act).astype(jnp.bfloat16)
    d_out_weight = jnp.dot(d_input.T, gated, preferred_element_type=jnp.float32)
    block_shape = (NBLK, BLOCK, GROUPS, HPG, HEAD_DIM)
    grad_y = (back_proj * gate_act).reshape(block_shape)
    inputs_x = values.astype(jnp.float32).reshape(block_shape)
    log_rate = log_decay.T.reshape(NBLK, BLOCK, GROUPS, HPG)
    write_rows = write_keys.astype(jnp.float32).reshape(NBLK, BLOCK, GROUPS, STATE)
    read_rows = read_keys.astype(jnp.float32).reshape(NBLK, BLOCK, GROUPS, STATE)
    start_states = entry_states.reshape(NBLK, GROUPS, HPG, HEAD_DIM, STATE)
    initial = jnp.zeros((GROUPS, HPG, HEAD_DIM, STATE), jnp.float32)
    final_state, outputs = lax.scan(block_back, initial, (inputs_x, grad_y, log_rate, write_rows, read_rows, start_states), reverse=True)
    grad_x, grad_w, grad_r = outputs
    d_values = grad_x.reshape(TOKENS, D_INNER).astype(jnp.bfloat16)
    d_write = grad_w.reshape(TOKENS, GROUPS * STATE)
    d_read = grad_r.reshape(TOKENS, GROUPS * STATE)
    return (grad_wg, grad_wu, grad_down, d_out_weight, d_input, d_values, d_write, d_read, d_gate)
```

```python
import functools

import jax
import jax.numpy as jnp
from jax import lax
from jax.experimental import pallas as pl
from jax.experimental.pallas import tpu as pltpu
from jax.sharding import PartitionSpec as P

D = 2048
HEAD_DIM = 64
BLOCK = 128
TOPK = 2
TOK_DEV = 128


precise = lax.Precision.HIGHEST


MESH_ID = pl.DeviceIdType.MESH
VMEM = pl.BlockSpec(memory_space=pltpu.VMEM)


def cols(t, width):
    return pl.ds(pl.multiple_of(t * width, width), width)


def signed_step(i):
    return (i // 2 + 1) * (1 - 2 * (i % 2))


def greet(n, m, me, t):
    barrier = pltpu.get_barrier_semaphore()

    @pl.loop(1, n)
    def _(d):
        pl.semaphore_signal(barrier, inc=1, device_id=((me + d) % n, t), device_id_type=MESH_ID)

    @pl.loop(1, m // 2)
    def _(d):
        pl.semaphore_signal(barrier, inc=1, device_id=(me, (t + 2 * d) % m), device_id_type=MESH_ID)

    pl.semaphore_signal(barrier, inc=1, device_id=(me, sibling(t)), device_id_type=MESH_ID)
    pl.semaphore_wait(barrier, n - 1 + m // 2)


def sibling(t):
    return t + 1 - 2 * (t % 2)


def remote(src, dst, send_sem, recv_sem, device):
    return pltpu.make_async_remote_copy(
        src_ref=src,
        dst_ref=dst,
        send_sem=send_sem,
        recv_sem=recv_sem,
        device_id=device,
        device_id_type=MESH_ID,
    )


class Spread:
    def __init__(self, n, m, me, t, buf, place, sems):
        self.n, self.m, self.me, self.t = n, m, me, t
        self.buf, self.place = buf, place
        self.recv, self.first, self.share, self.relay, self.own = sems

    @staticmethod
    def scratch(n, m):
        dma = pltpu.SemaphoreType.DMA
        return [dma((n, m)), dma((n,)), dma((n, m // 2)), dma((n, m // 2)), dma((1,))]

    def across(self, p):
        me, t = self.me, self.t
        return remote(
            self.buf.at[p], self.place(me, t), self.first.at[p], self.recv.at[me, t], (p, t)
        )

    def arrived(self, j, t):
        spot = self.place(j, t)
        remote(spot, spot, self.first.at[0], self.recv.at[j, t], (self.me, self.t)).wait_recv()

    def source(self, j, own):
        return self.buf.at[j] if own else self.place(j, self.t)

    def shared(self, j, d, own):
        me, t, m = self.me, self.t, self.m
        target = sibling(t) if d == 0 else (t + 2 * d) % m
        return remote(
            self.source(j, own),
            self.place(j, t),
            self.share.at[j, d],
            self.recv.at[j, t],
            (me, target),
        )

    def relayed(self, j, d):
        me, t, m = self.me, self.t, self.m
        origin = (t + 2 * d) % m
        spot = self.place(j, origin)
        return remote(spot, spot, self.relay.at[j, d], self.recv.at[j, origin], (me, sibling(t)))

    def mine(self):
        return pltpu.make_async_copy(
            self.buf.at[self.me], self.place(self.me, self.t), self.own.at[0]
        )

    def begin(self):
        @pl.loop(0, self.n - 1)
        def _(i):
            self.across((self.me + signed_step(i) + self.n) % self.n).start()

    def begin_own(self):
        for d in range(1, self.m // 2):
            self.shared(self.me, d, True).start()
        self.shared(self.me, 0, True).start()
        self.mine().start()

    def origin_of(self, i):
        return (self.me - signed_step(i) + self.n) % self.n

    def hand_on(self):
        half = self.m // 2

        def relay(j):
            for d in range(1, half):
                self.arrived(j, (self.t + 2 * d) % self.m)
                self.relayed(j, d).start()

        @pl.loop(0, self.n - 1)
        def _(i):
            j = self.origin_of(i)
            self.arrived(j, self.t)
            for d in range(1, half):
                self.shared(j, d, False).start()
            self.shared(j, 0, False).start()

            @pl.when(i == 0)
            def _():
                relay(self.me)

            @pl.when(i > 0)
            def _():
                relay(self.origin_of(i - 1))

        relay(self.origin_of(self.n - 2))

    def finish(self):
        n, m, half = self.n, self.m, self.m // 2
        self.mine().wait()
        for d in range(half):
            self.shared(self.me, d, True).wait_send()

        @pl.loop(0, n - 1)
        def _(i):
            self.across((self.me + signed_step(i) + n) % n).wait_send()
            j = self.origin_of(i)
            for d in range(half):
                self.shared(j, d, False).wait_send()

        @pl.loop(0, n)
        def _(j):
            for d in range(1, half):
                self.relayed(j, d).wait_send()
            for d in range(half):
                self.arrived(j, (sibling(self.t) + 2 * d) % m)


def dispatch_kernel(n, m, tok_ref, cot_ref, tok_out, cot_out, *sems):
    me, t = lax.axis_index("sp"), lax.axis_index("tp")
    width = tok_ref.shape[2]
    half = len(sems) // 2
    tok = Spread(n, m, me, t, tok_ref, lambda j, q: tok_out.at[j, :, cols(q, width)], sems[:half])
    cot = Spread(n, m, me, t, cot_ref, lambda j, q: cot_out.at[j, :, cols(q, width)], sems[half:])
    greet(n, m, me, t)
    tok.begin()
    tok.begin_own()
    cot.begin()
    cot.begin_own()
    tok.hand_on()
    cot.hand_on()
    tok.finish()
    cot.finish()


def dispatch(n, m, tok_buffer, cot_buffer):
    cap, width = tok_buffer.shape[1:]
    out = jax.ShapeDtypeStruct((n, cap, width * m), tok_buffer.dtype)
    return pl.pallas_call(
        functools.partial(dispatch_kernel, n, m),
        out_shape=(out, out),
        in_specs=[VMEM] * 2,
        out_specs=(VMEM, VMEM),
        scratch_shapes=Spread.scratch(n, m) * 2,
        compiler_params=pltpu.CompilerParams(collective_id=0, has_side_effects=True),
        name="dispatch",
    )(tok_buffer, cot_buffer)


def giveback_kernel(
    n, m, part_ref, pick_ref, cot_ref, gated_ref,
    whole_out, slice_out, gated_out,
    sib, away, near, leave, back,
    sib_send, sib_recv, away_send, near_recv, leave_send, back_recv,
    gated_send, gated_recv, gated_own, share_send, share_recv, relay_send,
):
    me, t = lax.axis_index("sp"), lax.axis_index("tp")
    half = m // 2
    width = cot_ref.shape[1]
    cap = part_ref.shape[1]
    other = sibling(t)
    f32 = jnp.float32
    greet(n, m, me, t)

    def to_sibling(d):
        return remote(
            part_ref.at[:, :, cols((other + 2 * d) % m, width)],
            sib.at[d],
            sib_send.at[d],
            sib_recv.at[d],
            (me, other),
        )

    def to_gated(p):
        return remote(gated_ref, gated_out.at[me], gated_send.at[p], gated_recv.at[me], (p, t))

    def to_column(j, d):
        return remote(
            away.at[d, j],
            near.at[d, j],
            away_send.at[d, j],
            near_recv.at[d, j],
            (me, (t + 2 * d) % m),
        )

    def to_home(j):
        return remote(leave.at[j], back.at[me], leave_send.at[j], back_recv.at[me], (j, t))

    order = lambda i: (me + signed_step(n - 2 - i) + n) % n

    for d in list(range(1, half)) + [0]:
        to_sibling(d).start()
    keep = pltpu.make_async_copy(gated_ref, gated_out.at[me], gated_own.at[0])
    keep.start()

    @pl.loop(0, n - 1)
    def _(i):
        to_gated(order(i)).start()

    for d in list(range(1, half)) + [0]:
        to_sibling(d).wait_recv()

    def pair_sum(j, d):
        q = (t + 2 * d) % m
        return part_ref[j, :, cols(q, width)].astype(f32) + sib[d, j].astype(f32)

    def fill(j):
        for d in range(1, half):
            away[d, j] = pair_sum(j, d).astype(jnp.bfloat16)

    def ship(j):
        for d in range(1, half):
            to_column(j, d).start()

    fill(order(0))

    @pl.loop(1, n - 1)
    def _(i):
        fill(order(i))
        ship(order(i - 1))

    fill(me)
    ship(order(n - 2))

    def total(j):
        acc = pair_sum(j, 0)
        for d in range(1, half):
            spot = near.at[d, j]
            remote(spot, spot, away_send.at[d, j], near_recv.at[d, j], (me, t)).wait_recv()
            acc = acc + near[d, j].astype(f32)
        return acc.astype(jnp.bfloat16)

    leave[order(0)] = total(order(0))
    ship(me)

    @pl.loop(1, n - 1)
    def _(i):
        leave[order(i)] = total(order(i))
        to_home(order(i - 1)).start()

    back[me] = total(me)
    to_home(order(n - 2)).start()

    @pl.loop(0, n - 1)
    def _(i):
        j = order(i)
        spot = back.at[j]
        remote(spot, spot, leave_send.at[j], back_recv.at[j], (me, t)).wait_recv()

    added = jnp.dot(pick_ref[...], back[...].reshape(n * cap, width), preferred_element_type=f32)
    result = (cot_ref[...].astype(f32) + added).astype(jnp.bfloat16)
    slice_out[...] = result
    whole_out[:, cols(t, width)] = result

    def spread(d):
        return remote(
            slice_out,
            whole_out.at[:, cols(t, width)],
            share_send.at[d],
            share_recv.at[t],
            (me, other if d == 0 else (t + 2 * d) % m),
        )

    def relay(d):
        q = (t + 2 * d) % m
        spot = whole_out.at[:, cols(q, width)]
        return remote(spot, spot, relay_send.at[d], share_recv.at[q], (me, other))

    def landed(q):
        spot = whole_out.at[:, cols(q, width)]
        remote(spot, spot, share_send.at[0], share_recv.at[q], (me, t)).wait_recv()

    for d in list(range(1, half)) + [0]:
        spread(d).start()
    for d in range(1, half):
        landed((t + 2 * d) % m)
        relay(d).start()
    for d in range(half):
        landed((other + 2 * d) % m)
    for d in range(half):
        spread(d).wait_send()
        to_sibling(d).wait_send()
    for d in range(1, half):
        relay(d).wait_send()

    @pl.loop(0, n - 1)
    def _(i):
        j = order(i)
        to_gated(j).wait_send()
        to_home(j).wait_send()
        spot = gated_out.at[j]
        remote(spot, spot, gated_send.at[j], gated_recv.at[j], (me, t)).wait_recv()

    @pl.loop(0, n)
    def _(j):
        for d in range(1, half):
            to_column(j, d).wait_send()

    keep.wait()


def giveback(n, m, part, pick, cot_slice, gated):
    cap = part.shape[1]
    rows, width = cot_slice.shape
    half = m // 2
    bf16, dma = jnp.bfloat16, pltpu.SemaphoreType.DMA
    return pl.pallas_call(
        functools.partial(giveback_kernel, n, m),
        out_shape=(
            jax.ShapeDtypeStruct((rows, width * m), bf16),
            jax.ShapeDtypeStruct((rows, width), bf16),
            jax.ShapeDtypeStruct((n,) + gated.shape, bf16),
        ),
        in_specs=[VMEM] * 4,
        out_specs=(VMEM,) * 3,
        scratch_shapes=[
            pltpu.VMEM((half, n, cap, width), bf16),
            pltpu.VMEM((half, n, cap, width), bf16),
            pltpu.VMEM((half, n, cap, width), bf16),
            pltpu.VMEM((n, cap, width), bf16),
            pltpu.VMEM((n, cap, width), bf16),
            dma((half,)), dma((half,)), dma((half, n)), dma((half, n)), dma((n,)), dma((n,)),
            dma((n,)), dma((n,)), dma((1,)), dma((half,)), dma((m,)), dma((half,)),
        ],
        compiler_params=pltpu.CompilerParams(collective_id=1, has_side_effects=True),
        name="giveback",
    )(part, pick, cot_slice, gated)


def later_kernel(
    n, m, grad_ref, decay_ref, rows_ref, state_out, rows_out,
    held, rates, grad_send, grad_recv, rate_send, rate_recv, *sems,
):
    me, t = lax.axis_index("sp"), lax.axis_index("tp")
    rows = Spread(n, m, me, t, rows_ref, lambda j, q: rows_out.at[j, q], sems)
    greet(n, m, me, t)

    def grad_to(p):
        return remote(grad_ref, held.at[me], grad_send.at[p], grad_recv.at[me], (p, t))

    def rate_to(p):
        return remote(decay_ref, rates.at[me], rate_send.at[p], rate_recv.at[me], (p, t))

    rows.begin()
    rows.begin_own()

    @pl.loop(0, me)
    def _(p):
        rate_to(p).start()
        grad_to(p).start()

    rows.hand_on()
    state_out[...] = jnp.zeros_like(state_out)

    @pl.loop(0, n - 1 - me)
    def _(i):
        j = n - 1 - i
        spot, rate = held.at[j], rates.at[j]
        remote(rate, rate, rate_send.at[j], rate_recv.at[j], (me, t)).wait_recv()
        remote(spot, spot, grad_send.at[j], grad_recv.at[j], (me, t)).wait_recv()
        state_out[...] = rates[j][:, None, :] * state_out[...] + held[j].astype(jnp.float32)

    @pl.loop(0, me)
    def _(p):
        rate_to(p).wait_send()
        grad_to(p).wait_send()

    rows.finish()


def later(n, m, grad, decay, rows):
    dma = pltpu.SemaphoreType.DMA
    return pl.pallas_call(
        functools.partial(later_kernel, n, m),
        out_shape=(
            jax.ShapeDtypeStruct(grad.shape, jnp.float32),
            jax.ShapeDtypeStruct((n, m) + rows.shape[1:], rows.dtype),
        ),
        in_specs=[VMEM] * 3,
        out_specs=(VMEM,) * 2,
        scratch_shapes=[
            pltpu.VMEM((n,) + grad.shape, grad.dtype),
            pltpu.VMEM((n,) + decay.shape, decay.dtype),
            dma((n,)), dma((n,)), dma((n,)), dma((n,)),
        ] + Spread.scratch(n, m),
        compiler_params=pltpu.CompilerParams(collective_id=2, has_side_effects=True),
        name="later",
    )(grad, decay, rows)


def silu_grad(pre_act):
    logistic = jax.nn.sigmoid(pre_act)
    return logistic * (1.0 + pre_act * (1.0 - logistic))


def contract_rows(first_op, second_op):
    return lax.dot_general(
        first_op, second_op, (((0,), (0,)), ((), ())), preferred_element_type=jnp.float32
    )


def contract_cols(first_op, second_op):
    return lax.dot_general(
        first_op, second_op, (((1,), (1,)), ((), ())), preferred_element_type=jnp.float32
    )


def block_back(grad_state, inputs_x, grad_y, log_rate, write_rows, read_rows, start_state):
    block_len = log_rate.shape[0]
    running = jnp.cumsum(log_rate, axis=0)
    causal_mask = (jnp.arange(block_len)[:, None] >= jnp.arange(block_len)[None, :])[:, :, None]
    spread = running[:, None, :] - running[None, :, :]
    decay_mat = jnp.where(causal_mask, jnp.exp(jnp.where(causal_mask, spread, 0.0)), 0.0)
    intersection = jnp.dot(read_rows, write_rows.T, precision=precise)
    mixing = intersection[:, :, None] * decay_mat
    to_end = jnp.exp(running[-1][None, :] - running)
    from_start = jnp.exp(running)
    grad_x = jnp.einsum("lsj,ljp->sjp", mixing, grad_y, precision=precise) + to_end[
        :, :, None
    ] * jnp.einsum("sn,jpn->sjp", write_rows, grad_state, precision=precise)
    weighted = jnp.einsum("ljp,sjp->lsj", grad_y, inputs_x, precision=precise) * decay_mat
    grad_w = jnp.einsum("lsj,ln->sn", weighted, read_rows, precision=precise) + jnp.einsum(
        "sj,sjp,jpn->sn", to_end, inputs_x, grad_state, precision=precise
    )
    grad_r = jnp.einsum("lsj,sn->ln", weighted, write_rows, precision=precise) + jnp.einsum(
        "lj,ljp,jpn->ln", from_start, grad_y, start_state, precision=precise
    )
    earlier = jnp.exp(running[-1])[:, None, None] * grad_state + jnp.einsum(
        "lj,ljp,ln->jpn", from_start, grad_y, read_rows, precision=precise
    )
    return (earlier, grad_x, grad_w, grad_r)


def body(
    mixed,
    cotangent,
    routes,
    gates,
    w_gate,
    w_up,
    w_down,
    out_weight,
    gate_pre,
    mixer_out,
    values,
    write_keys,
    read_keys,
    log_decay,
    entry_states,
):
    sp_count = lax.axis_size("sp")
    tp_count = lax.axis_size("tp")
    capacity = 4 * TOK_DEV // sp_count
    assigned = TOK_DEV * TOPK
    picks = routes.reshape(assigned)
    onehot = (picks[:, None] == jnp.arange(sp_count, dtype=jnp.int32)[None, :]).astype(jnp.int32)
    earlier_same = jnp.cumsum(onehot, axis=0) - onehot
    slot_of = jnp.sum(earlier_same * onehot, axis=1)
    target = (picks * capacity + slot_of).reshape(TOK_DEV, TOPK)
    slots = jnp.arange(sp_count * capacity, dtype=jnp.int32)[None, :]
    chosen = [(target[:, k : k + 1] == slots).astype(jnp.bfloat16) for k in range(TOPK)]
    pick = sum(chosen[1:], chosen[0])
    weight_g = w_gate[0]
    weight_u = w_up[0]
    weight_d = w_down[0]
    column_count = D // tp_count
    offset = lax.axis_index("tp") * column_count
    tok_slice = lax.dynamic_slice_in_dim(mixed, offset, column_count, 1)
    cot_slice = lax.dynamic_slice_in_dim(cotangent, offset, column_count, 1)
    scaled = [
        (gates[:, k : k + 1] * cot_slice.astype(jnp.float32)).astype(jnp.bfloat16)
        for k in range(TOPK)
    ]
    tok_buffer = contract_rows(pick, tok_slice).astype(jnp.bfloat16)
    cot_buffer = contract_rows(
        jnp.concatenate(chosen, axis=0), jnp.concatenate(scaled, axis=0)
    ).astype(jnp.bfloat16)
    expert_tok_rows, expert_cot_rows = dispatch(
        sp_count,
        tp_count,
        tok_buffer.reshape(sp_count, capacity, column_count),
        cot_buffer.reshape(sp_count, capacity, column_count),
    )
    expert_tok_rows = expert_tok_rows.reshape(-1, D)
    expert_cot_rows = expert_cot_rows.reshape(-1, D)
    pre_gate = jnp.dot(expert_tok_rows, weight_g, preferred_element_type=jnp.float32)
    pre_up = jnp.dot(expert_tok_rows, weight_u, preferred_element_type=jnp.float32)
    active = jax.nn.silu(pre_gate)
    hidden = (active * pre_up).astype(jnp.bfloat16)
    grad_down = contract_rows(hidden, expert_cot_rows)
    grad_hidden = contract_cols(expert_cot_rows, weight_d)
    grad_gate = (grad_hidden * pre_up * silu_grad(pre_gate)).astype(jnp.bfloat16)
    grad_upval = (grad_hidden * active).astype(jnp.bfloat16)
    grad_wg = contract_rows(expert_tok_rows, grad_gate)
    grad_wu = contract_rows(expert_tok_rows, grad_upval)
    partial_value = contract_cols(grad_gate, weight_g) + contract_cols(grad_upval, weight_u)
    pre_act = gate_pre.astype(jnp.float32)
    gate_act = jax.nn.silu(pre_act)
    saved_out = mixer_out.astype(jnp.float32)
    gated = (saved_out * gate_act).astype(jnp.bfloat16)
    whole, d_input, all_gated = giveback(
        sp_count,
        tp_count,
        partial_value.astype(jnp.bfloat16).reshape(sp_count, capacity, D),
        pick,
        cot_slice,
        gated,
    )
    back_proj = contract_cols(whole, out_weight)
    d_gate = (back_proj * saved_out * silu_grad(pre_act)).astype(jnp.bfloat16)
    head_count = out_weight.shape[0] // HEAD_DIM
    grad_y = (back_proj * gate_act).reshape(TOK_DEV, head_count, HEAD_DIM)
    inputs_x = values.astype(jnp.float32).reshape(TOK_DEV, head_count, HEAD_DIM)
    write_rows = write_keys.astype(jnp.float32)
    read_rows = read_keys.astype(jnp.float32)
    log_rate = log_decay.T
    total_run = jnp.cumsum(log_rate, axis=0)
    shard_decay = jnp.exp(total_run[-1])
    shard_grad = jnp.einsum(
        "lj,ljp,ln->jpn", jnp.exp(total_run), grad_y, read_rows, precision=precise
    )
    share = TOK_DEV // tp_count
    own_rows = lax.dynamic_slice_in_dim(whole, lax.axis_index("tp") * share, share, 0)
    own_rows = own_rows.reshape(share, sp_count, D // sp_count).transpose(1, 0, 2)
    grad_state, all_rows = later(
        sp_count,
        tp_count,
        shard_grad.astype(jnp.bfloat16),
        jnp.broadcast_to(shard_decay[:, None], (head_count, shard_grad.shape[2])),
        own_rows,
    )
    d_out_weight = contract_rows(
        all_rows.reshape(sp_count * TOK_DEV, D // sp_count),
        all_gated.reshape(sp_count * TOK_DEV, all_gated.shape[2]),
    )
    pieces_x = []
    pieces_w = []
    pieces_r = []
    for block_id in reversed(range(TOK_DEV // BLOCK)):
        grad_state, grad_x, grad_w, grad_r = block_back(
            grad_state, inputs_x, grad_y, log_rate, write_rows, read_rows, entry_states[block_id]
        )
        pieces_x.insert(0, grad_x)
        pieces_w.insert(0, grad_w)
        pieces_r.insert(0, grad_r)
    d_values = pieces_x[0].reshape(TOK_DEV, head_count * HEAD_DIM).astype(jnp.bfloat16)
    d_write = pieces_w[0]
    d_read = pieces_r[0]
    return (
        grad_wg.astype(jnp.bfloat16)[None],
        grad_wu.astype(jnp.bfloat16)[None],
        grad_down.astype(jnp.bfloat16)[None],
        d_out_weight,
        d_input,
        d_values,
        d_write,
        d_read,
        d_gate,
    )


def solution(mesh):
    return jax.shard_map(
        body,
        mesh=mesh,
        in_specs=(
            P("sp", None),
            P("sp", None),
            P("sp", None),
            P("sp", None),
            P("sp", None, "tp"),
            P("sp", None, "tp"),
            P("sp", "tp", None),
            P("tp", None),
            P("sp", "tp"),
            P("sp", "tp"),
            P("sp", "tp"),
            P("sp", "tp"),
            P("sp", "tp"),
            P("tp", "sp"),
            P("sp", "tp", None, None),
        ),
        out_specs=(
            P("sp", None, "tp"),
            P("sp", None, "tp"),
            P("sp", "tp", None),
            P("sp", "tp"),
            P("sp", "tp"),
            P("sp", "tp"),
            P("sp", "tp"),
            P("sp", "tp"),
            P("sp", "tp"),
        ),
        check_vma=False,
    )
```

```python
import functools

import jax
import jax.numpy as jnp
from jax import lax
from jax.experimental import pallas as pl
from jax.experimental.pallas import tpu as pltpu
from jax.sharding import PartitionSpec as P

D = 2048
HEAD_DIM = 64
BLOCK = 128
TOPK = 2
TOK_DEV = 128


precise = lax.Precision.HIGHEST


MESH_ID = pl.DeviceIdType.MESH
VMEM = pl.BlockSpec(memory_space=pltpu.VMEM)


def cols(t, width):
    return pl.ds(pl.multiple_of(t * width, width), width)


def signed_step(i):
    return (i // 2 + 1) * (1 - 2 * (i % 2))


def announce(n, m, me, t):
    barrier = pltpu.get_barrier_semaphore()

    @pl.loop(1, n)
    def _(d):
        pl.semaphore_signal(barrier, inc=1, device_id=((me + d) % n, t), device_id_type=MESH_ID)

    @pl.loop(1, m // 2)
    def _(d):
        pl.semaphore_signal(barrier, inc=1, device_id=(me, (t + 2 * d) % m), device_id_type=MESH_ID)

    pl.semaphore_signal(barrier, inc=1, device_id=(me, sibling(t)), device_id_type=MESH_ID)


def await_all(n, m):
    pl.semaphore_wait(pltpu.get_barrier_semaphore(), n - 1 + m // 2)


def greet(n, m, me, t):
    announce(n, m, me, t)
    await_all(n, m)


def sibling(t):
    return t + 1 - 2 * (t % 2)


def remote(src, dst, send_sem, recv_sem, device):
    return pltpu.make_async_remote_copy(
        src_ref=src,
        dst_ref=dst,
        send_sem=send_sem,
        recv_sem=recv_sem,
        device_id=device,
        device_id_type=MESH_ID,
    )


class Spread:
    def __init__(self, n, m, me, t, buf, place, sems):
        self.n, self.m, self.me, self.t = n, m, me, t
        self.buf, self.place = buf, place
        self.recv, self.first, self.share, self.relay, self.own = sems

    @staticmethod
    def scratch(n, m):
        dma = pltpu.SemaphoreType.DMA
        return [dma((n, m)), dma((n,)), dma((n, m // 2)), dma((n, m // 2)), dma((1,))]

    def across(self, p):
        me, t = self.me, self.t
        return remote(
            self.buf.at[p], self.place(me, t), self.first.at[p], self.recv.at[me, t], (p, t)
        )

    def arrived(self, j, t):
        spot = self.place(j, t)
        remote(spot, spot, self.first.at[0], self.recv.at[j, t], (self.me, self.t)).wait_recv()

    def source(self, j, own):
        return self.buf.at[j] if own else self.place(j, self.t)

    def shared(self, j, d, own):
        me, t, m = self.me, self.t, self.m
        target = sibling(t) if d == 0 else (t + 2 * d) % m
        return remote(
            self.source(j, own),
            self.place(j, t),
            self.share.at[j, d],
            self.recv.at[j, t],
            (me, target),
        )

    def relayed(self, j, d):
        me, t, m = self.me, self.t, self.m
        origin = (t + 2 * d) % m
        spot = self.place(j, origin)
        return remote(spot, spot, self.relay.at[j, d], self.recv.at[j, origin], (me, sibling(t)))

    def mine(self):
        return pltpu.make_async_copy(
            self.buf.at[self.me], self.place(self.me, self.t), self.own.at[0]
        )

    def begin(self):
        @pl.loop(0, self.n - 1)
        def _(i):
            self.across((self.me + signed_step(i) + self.n) % self.n).start()

    def begin_own(self):
        for d in range(1, self.m // 2):
            self.shared(self.me, d, True).start()
        self.shared(self.me, 0, True).start()
        self.mine().start()

    def origin_of(self, i):
        return (self.me - signed_step(i) + self.n) % self.n

    def hand_on(self):
        half = self.m // 2

        def relay(j):
            for d in range(1, half):
                self.arrived(j, (self.t + 2 * d) % self.m)
                self.relayed(j, d).start()

        @pl.loop(0, self.n - 1)
        def _(i):
            j = self.origin_of(i)
            self.arrived(j, self.t)
            for d in range(1, half):
                self.shared(j, d, False).start()
            self.shared(j, 0, False).start()

            @pl.when(i == 0)
            def _():
                relay(self.me)

            @pl.when(i > 0)
            def _():
                relay(self.origin_of(i - 1))

        relay(self.origin_of(self.n - 2))

    def finish(self):
        n, m, half = self.n, self.m, self.m // 2
        self.mine().wait()
        for d in range(half):
            self.shared(self.me, d, True).wait_send()

        @pl.loop(0, n - 1)
        def _(i):
            self.across((self.me + signed_step(i) + n) % n).wait_send()
            j = self.origin_of(i)
            for d in range(half):
                self.shared(j, d, False).wait_send()

        @pl.loop(0, n)
        def _(j):
            for d in range(1, half):
                self.relayed(j, d).wait_send()
            for d in range(half):
                self.arrived(j, (sibling(self.t) + 2 * d) % m)


def dispatch_kernel(
    n, m, mixed_ref, cot_ref, routes_ref, gates_ref,
    tok_out, cot_out, pick_out, tok_buf, cot_buf, *sems,
):
    me, t = lax.axis_index("sp"), lax.axis_index("tp")
    f32, bf16 = jnp.float32, jnp.bfloat16
    cap, width = tok_buf.shape[1:]
    half = len(sems) // 2
    announce(n, m, me, t)
    routes, gates = routes_ref[...], gates_ref[...]
    rows = routes.shape[0]
    expert = lax.broadcasted_iota(jnp.int32, (rows, n), 1)
    hot = [(routes[:, k : k + 1] == expert).astype(f32) for k in range(TOPK)]
    later = lax.broadcasted_iota(jnp.int32, (rows, rows), 0)
    sooner = lax.broadcasted_iota(jnp.int32, (rows, rows), 1)
    counts = jnp.dot(
        (later > sooner).astype(bf16), sum(hot[1:], hot[0]).astype(bf16), preferred_element_type=f32
    )
    slots = lax.broadcasted_iota(jnp.int32, (rows, n * cap), 1).astype(f32)
    chosen = []
    for k in range(TOPK):
        slot = jnp.sum(hot[k] * counts, axis=1, keepdims=True)
        target = routes[:, k : k + 1].astype(f32) * cap + slot
        chosen.append((target == slots).astype(f32).astype(bf16))
        counts = counts + hot[k]
    pick = sum(chosen[1:], chosen[0])
    tok = contract_rows(pick, mixed_ref[:, cols(t, width)])
    tok_buf[...] = tok.astype(bf16).reshape(n, cap, width)
    cotangent = cot_ref[:, cols(t, width)].astype(f32)
    scaled = [(gates[:, k : k + 1] * cotangent).astype(bf16) for k in range(TOPK)]
    cot = sum(contract_rows(chosen[k], scaled[k]) for k in range(TOPK))
    cot_buf[...] = cot.astype(bf16).reshape(n, cap, width)
    pick_out[...] = pick
    tok = Spread(n, m, me, t, tok_buf, lambda j, q: tok_out.at[j, :, cols(q, width)], sems[:half])
    cot = Spread(n, m, me, t, cot_buf, lambda j, q: cot_out.at[j, :, cols(q, width)], sems[half:])
    await_all(n, m)
    tok.begin()
    tok.begin_own()
    cot.begin()
    cot.begin_own()
    tok.hand_on()
    cot.hand_on()
    tok.finish()
    cot.finish()


def dispatch(n, m, cap, mixed, cotangent, routes, gates):
    rows, depth = mixed.shape
    bf16 = jnp.bfloat16
    out = jax.ShapeDtypeStruct((n, cap, depth), bf16)
    return pl.pallas_call(
        functools.partial(dispatch_kernel, n, m),
        out_shape=(out, out, jax.ShapeDtypeStruct((rows, n * cap), bf16)),
        in_specs=[VMEM] * 4,
        out_specs=(VMEM,) * 3,
        scratch_shapes=[pltpu.VMEM((n, cap, depth // m), bf16)] * 2 + Spread.scratch(n, m) * 2,
        compiler_params=pltpu.CompilerParams(collective_id=0, has_side_effects=True),
        name="dispatch",
    )(mixed, cotangent, routes, gates)


def giveback_kernel(
    n, m, part_ref, pick_ref, cot_ref, gated_ref,
    whole_out, slice_out, gated_out,
    sib, away, near, leave, back,
    sib_send, sib_recv, away_send, near_recv, leave_send, back_recv,
    gated_send, gated_recv, gated_own, gated_relay, share_send, share_recv, relay_send,
):
    me, t = lax.axis_index("sp"), lax.axis_index("tp")
    half = m // 2
    width = cot_ref.shape[1] // m
    cap = part_ref.shape[1]
    other = sibling(t)
    f32 = jnp.float32
    greet(n, m, me, t)

    def to_sibling(d):
        return remote(
            part_ref.at[:, :, cols((other + 2 * d) % m, width)],
            sib.at[d],
            sib_send.at[d],
            sib_recv.at[d],
            (me, other),
        )

    def to_gated(p):
        return remote(gated_ref, gated_out.at[me], gated_send.at[p], gated_recv.at[me], (p, t))

    def to_column(j, d):
        return remote(
            away.at[d, j],
            near.at[d, j],
            away_send.at[d, j],
            near_recv.at[d, j],
            (me, (t + 2 * d) % m),
        )

    def to_home(j):
        return remote(leave.at[j], back.at[me], leave_send.at[j], back_recv.at[me], (j, t))

    def gated_on(j):
        spot = gated_out.at[j]
        return remote(spot, spot, gated_relay.at[j], gated_recv.at[j], (sibling(me), t))

    def gated_in(j):
        spot = gated_out.at[j]
        remote(spot, spot, gated_send.at[j], gated_recv.at[j], (me, t)).wait_recv()

    order = lambda i: (me + signed_step(n - 2 - i) + n) % n

    for d in list(range(1, half)) + [0]:
        to_sibling(d).start()
    keep = pltpu.make_async_copy(gated_ref, gated_out.at[me], gated_own.at[0])
    keep.start()

    to_gated(sibling(me)).start()

    @pl.loop(1, n // 2)
    def _(k):
        to_gated((me + 2 * k) % n).start()

    for d in list(range(1, half)) + [0]:
        to_sibling(d).wait_recv()

    def pair_sum(j, d):
        q = (t + 2 * d) % m
        return part_ref[j, :, cols(q, width)].astype(f32) + sib[d, j].astype(f32)

    def fill(j):
        for d in range(1, half):
            away[d, j] = pair_sum(j, d).astype(jnp.bfloat16)

    def ship(j):
        for d in range(1, half):
            to_column(j, d).start()

    fill(order(0))

    @pl.loop(1, n - 1)
    def _(i):
        fill(order(i))
        ship(order(i - 1))

    fill(me)
    ship(order(n - 2))

    def total(j):
        acc = pair_sum(j, 0)
        for d in range(1, half):
            spot = near.at[d, j]
            remote(spot, spot, away_send.at[d, j], near_recv.at[d, j], (me, t)).wait_recv()
            acc = acc + near[d, j].astype(f32)
        return acc.astype(jnp.bfloat16)

    leave[order(0)] = total(order(0))
    ship(me)

    @pl.loop(1, n - 1)
    def _(i):
        leave[order(i)] = total(order(i))
        to_home(order(i - 1)).start()

    back[me] = total(me)
    to_home(order(n - 2)).start()

    @pl.loop(1, n // 2)
    def _(k):
        j = (me - 2 * k + n) % n
        gated_in(j)
        gated_on(j).start()

    @pl.loop(0, n - 1)
    def _(i):
        j = order(i)
        spot = back.at[j]
        remote(spot, spot, leave_send.at[j], back_recv.at[j], (me, t)).wait_recv()

    added = jnp.dot(pick_ref[...], back[...].reshape(n * cap, width), preferred_element_type=f32)
    result = (cot_ref[:, cols(t, width)].astype(f32) + added).astype(jnp.bfloat16)
    slice_out[...] = result
    whole_out[:, cols(t, width)] = result

    def spread(d):
        return remote(
            slice_out,
            whole_out.at[:, cols(t, width)],
            share_send.at[d],
            share_recv.at[t],
            (me, other if d == 0 else (t + 2 * d) % m),
        )

    def relay(d):
        q = (t + 2 * d) % m
        spot = whole_out.at[:, cols(q, width)]
        return remote(spot, spot, relay_send.at[d], share_recv.at[q], (me, other))

    def landed(q):
        spot = whole_out.at[:, cols(q, width)]
        remote(spot, spot, share_send.at[0], share_recv.at[q], (me, t)).wait_recv()

    for d in list(range(1, half)) + [0]:
        spread(d).start()
    for d in range(1, half):
        landed((t + 2 * d) % m)
        relay(d).start()
    for d in range(half):
        landed((other + 2 * d) % m)
    for d in range(half):
        spread(d).wait_send()
        to_sibling(d).wait_send()
    for d in range(1, half):
        relay(d).wait_send()

    @pl.loop(0, n - 1)
    def _(i):
        j = order(i)
        to_home(j).wait_send()

    to_gated(sibling(me)).wait_send()
    gated_in(sibling(me))

    @pl.loop(1, n // 2)
    def _(k):
        to_gated((me + 2 * k) % n).wait_send()
        gated_on((me - 2 * k + n) % n).wait_send()
        gated_in((sibling(me) + 2 * k) % n)

    @pl.loop(0, n)
    def _(j):
        for d in range(1, half):
            to_column(j, d).wait_send()

    keep.wait()


def giveback(n, m, part, pick, cotangent, gated):
    cap = part.shape[1]
    rows, width = cotangent.shape[0], cotangent.shape[1] // m
    half = m // 2
    bf16, dma = jnp.bfloat16, pltpu.SemaphoreType.DMA
    return pl.pallas_call(
        functools.partial(giveback_kernel, n, m),
        out_shape=(
            jax.ShapeDtypeStruct((rows, width * m), bf16),
            jax.ShapeDtypeStruct((rows, width), bf16),
            jax.ShapeDtypeStruct((n,) + gated.shape, bf16),
        ),
        in_specs=[VMEM] * 4,
        out_specs=(VMEM,) * 3,
        scratch_shapes=[
            pltpu.VMEM((half, n, cap, width), bf16),
            pltpu.VMEM((half, n, cap, width), bf16),
            pltpu.VMEM((half, n, cap, width), bf16),
            pltpu.VMEM((n, cap, width), bf16),
            pltpu.VMEM((n, cap, width), bf16),
            dma((half,)), dma((half,)), dma((half, n)), dma((half, n)), dma((n,)), dma((n,)),
            dma((n,)), dma((n,)), dma((1,)), dma((n,)), dma((half,)), dma((m,)), dma((half,)),
        ],
        compiler_params=pltpu.CompilerParams(collective_id=1, has_side_effects=True),
        name="giveback",
    )(part, pick, cotangent, gated)


def later_kernel(
    n, m, grad_ref, decay_ref, rows_ref, state_out, rows_out,
    held, rates, near, far, grad_send, grad_recv, rate_send, rate_recv, pair_send, pair_recv, *sems,
):
    me, t = lax.axis_index("sp"), lax.axis_index("tp")
    rows = Spread(n, m, me, t, rows_ref, lambda j, q: rows_out.at[j, q], sems)
    greet(n, m, me, t)

    def grad_to(p):
        return remote(grad_ref, held.at[me], grad_send.at[p], grad_recv.at[me], (p, t))

    def rate_to(p):
        return remote(decay_ref, rates.at[me], rate_send.at[p], rate_recv.at[me], (p, t))

    def grad_in(j):
        spot = held.at[j]
        remote(spot, spot, grad_send.at[j], grad_recv.at[j], (me, t)).wait_recv()

    odd = me % 2

    @pl.loop(0, me)
    def _(p):
        rate_to(p).start()

    @pl.when(odd == 1)
    def _():
        grad_to(me - 1).start()

    @pl.loop(1, me // 2 + 1)
    def _(k):
        grad_to(me - 2 * k).start()

    rows.begin()
    rows.begin_own()
    rows.hand_on()
    state_out[...] = jnp.zeros_like(state_out)

    @pl.loop(me + 1, n)
    def _(j):
        rate = rates.at[j]
        remote(rate, rate, rate_send.at[j], rate_recv.at[j], (me, t)).wait_recv()

    @pl.loop(0, n // 2 - 1 - me // 2)
    def _(i):
        even = n - 2 - 2 * i
        j = even + odd
        grad_in(j)
        first, second = rates[even], rates[even + 1]
        lead = jnp.where(odd == 1, first, jnp.ones_like(first))
        state_out[...] = (first * second)[:, None, :] * state_out[...] + lead[
            :, None, :
        ] * held[j].astype(jnp.float32)

    near[...] = state_out[...].astype(near.dtype)
    swap = remote(near, far, pair_send.at[0], pair_recv.at[0], (sibling(me), t))
    swap.start()
    swap.wait()
    state_out[...] = state_out[...] + far[...].astype(jnp.float32)

    @pl.when(odd == 0)
    def _():
        grad_in(me + 1)
        state_out[...] = rates[me + 1][:, None, :] * state_out[...] + held[me + 1].astype(
            jnp.float32
        )

    @pl.loop(0, me)
    def _(p):
        rate_to(p).wait_send()

    @pl.when(odd == 1)
    def _():
        grad_to(me - 1).wait_send()

    @pl.loop(1, me // 2 + 1)
    def _(k):
        grad_to(me - 2 * k).wait_send()

    rows.finish()


def later(n, m, grad, decay, rows):
    dma = pltpu.SemaphoreType.DMA
    return pl.pallas_call(
        functools.partial(later_kernel, n, m),
        out_shape=(
            jax.ShapeDtypeStruct(grad.shape, jnp.float32),
            jax.ShapeDtypeStruct((n, m) + rows.shape[1:], rows.dtype),
        ),
        in_specs=[VMEM] * 3,
        out_specs=(VMEM,) * 2,
        scratch_shapes=[
            pltpu.VMEM((n,) + grad.shape, grad.dtype),
            pltpu.VMEM((n,) + decay.shape, decay.dtype),
            pltpu.VMEM(grad.shape, grad.dtype),
            pltpu.VMEM(grad.shape, grad.dtype),
            dma((n,)), dma((n,)), dma((n,)), dma((n,)), dma((1,)), dma((1,)),
        ] + Spread.scratch(n, m),
        compiler_params=pltpu.CompilerParams(collective_id=2, has_side_effects=True),
        name="later",
    )(grad, decay, rows)


def silu_grad(pre_act):
    logistic = jax.nn.sigmoid(pre_act)
    return logistic * (1.0 + pre_act * (1.0 - logistic))


def contract_rows(first_op, second_op):
    return lax.dot_general(
        first_op, second_op, (((0,), (0,)), ((), ())), preferred_element_type=jnp.float32
    )


def contract_cols(first_op, second_op):
    return lax.dot_general(
        first_op, second_op, (((1,), (1,)), ((), ())), preferred_element_type=jnp.float32
    )


def block_back(grad_state, inputs_x, grad_y, log_rate, write_rows, read_rows, start_state):
    block_len = log_rate.shape[0]
    running = jnp.cumsum(log_rate, axis=0)
    causal_mask = (jnp.arange(block_len)[:, None] >= jnp.arange(block_len)[None, :])[:, :, None]
    spread = running[:, None, :] - running[None, :, :]
    decay_mat = jnp.where(causal_mask, jnp.exp(jnp.where(causal_mask, spread, 0.0)), 0.0)
    intersection = jnp.dot(read_rows, write_rows.T, precision=precise)
    mixing = intersection[:, :, None] * decay_mat
    to_end = jnp.exp(running[-1][None, :] - running)
    from_start = jnp.exp(running)
    grad_x = jnp.einsum("lsj,ljp->sjp", mixing, grad_y, precision=precise) + to_end[
        :, :, None
    ] * jnp.einsum("sn,jpn->sjp", write_rows, grad_state, precision=precise)
    weighted = jnp.einsum("ljp,sjp->lsj", grad_y, inputs_x, precision=precise) * decay_mat
    grad_w = jnp.einsum("lsj,ln->sn", weighted, read_rows, precision=precise) + jnp.einsum(
        "sj,sjp,jpn->sn", to_end, inputs_x, grad_state, precision=precise
    )
    grad_r = jnp.einsum("lsj,sn->ln", weighted, write_rows, precision=precise) + jnp.einsum(
        "lj,ljp,jpn->ln", from_start, grad_y, start_state, precision=precise
    )
    earlier = jnp.exp(running[-1])[:, None, None] * grad_state + jnp.einsum(
        "lj,ljp,ln->jpn", from_start, grad_y, read_rows, precision=precise
    )
    return (earlier, grad_x, grad_w, grad_r)


def body(
    mixed,
    cotangent,
    routes,
    gates,
    w_gate,
    w_up,
    w_down,
    out_weight,
    gate_pre,
    mixer_out,
    values,
    write_keys,
    read_keys,
    log_decay,
    entry_states,
):
    sp_count = lax.axis_size("sp")
    tp_count = lax.axis_size("tp")
    capacity = 4 * TOK_DEV // sp_count
    weight_g = w_gate[0]
    weight_u = w_up[0]
    weight_d = w_down[0]
    expert_tok_rows, expert_cot_rows, pick = dispatch(
        sp_count, tp_count, capacity, mixed, cotangent, routes, gates
    )
    expert_tok_rows = expert_tok_rows.reshape(-1, D)
    expert_cot_rows = expert_cot_rows.reshape(-1, D)
    pre_gate = jnp.dot(expert_tok_rows, weight_g, preferred_element_type=jnp.float32)
    pre_up = jnp.dot(expert_tok_rows, weight_u, preferred_element_type=jnp.float32)
    active = jax.nn.silu(pre_gate)
    hidden = (active * pre_up).astype(jnp.bfloat16)
    grad_down = contract_rows(hidden, expert_cot_rows)
    grad_hidden = contract_cols(expert_cot_rows, weight_d)
    grad_gate = (grad_hidden * pre_up * silu_grad(pre_gate)).astype(jnp.bfloat16)
    grad_upval = (grad_hidden * active).astype(jnp.bfloat16)
    grad_wg = contract_rows(expert_tok_rows, grad_gate)
    grad_wu = contract_rows(expert_tok_rows, grad_upval)
    partial_value = contract_cols(grad_gate, weight_g) + contract_cols(grad_upval, weight_u)
    pre_act = gate_pre.astype(jnp.float32)
    gate_act = jax.nn.silu(pre_act)
    saved_out = mixer_out.astype(jnp.float32)
    gated = (saved_out * gate_act).astype(jnp.bfloat16)
    whole, d_input, all_gated = giveback(
        sp_count,
        tp_count,
        partial_value.astype(jnp.bfloat16).reshape(sp_count, capacity, D),
        pick,
        cotangent,
        gated,
    )
    back_proj = contract_cols(whole, out_weight)
    d_gate = (back_proj * saved_out * silu_grad(pre_act)).astype(jnp.bfloat16)
    head_count = out_weight.shape[0] // HEAD_DIM
    grad_y = (back_proj * gate_act).reshape(TOK_DEV, head_count, HEAD_DIM)
    inputs_x = values.astype(jnp.float32).reshape(TOK_DEV, head_count, HEAD_DIM)
    write_rows = write_keys.astype(jnp.float32)
    read_rows = read_keys.astype(jnp.float32)
    log_rate = log_decay.T
    total_run = jnp.cumsum(log_rate, axis=0)
    shard_decay = jnp.exp(total_run[-1])
    shard_grad = jnp.einsum(
        "lj,ljp,ln->jpn", jnp.exp(total_run), grad_y, read_rows, precision=precise
    )
    share = TOK_DEV // tp_count
    own_rows = lax.dynamic_slice_in_dim(whole, lax.axis_index("tp") * share, share, 0)
    own_rows = own_rows.reshape(share, sp_count, D // sp_count).transpose(1, 0, 2)
    grad_state, all_rows = later(
        sp_count,
        tp_count,
        shard_grad.astype(jnp.bfloat16),
        jnp.broadcast_to(shard_decay[:, None], (head_count, shard_grad.shape[2])),
        own_rows,
    )
    d_out_weight = contract_rows(
        all_rows.reshape(sp_count * TOK_DEV, D // sp_count),
        all_gated.reshape(sp_count * TOK_DEV, all_gated.shape[2]),
    )
    pieces_x = []
    pieces_w = []
    pieces_r = []
    for block_id in reversed(range(TOK_DEV // BLOCK)):
        grad_state, grad_x, grad_w, grad_r = block_back(
            grad_state, inputs_x, grad_y, log_rate, write_rows, read_rows, entry_states[block_id]
        )
        pieces_x.insert(0, grad_x)
        pieces_w.insert(0, grad_w)
        pieces_r.insert(0, grad_r)
    d_values = pieces_x[0].reshape(TOK_DEV, head_count * HEAD_DIM).astype(jnp.bfloat16)
    d_write = pieces_w[0]
    d_read = pieces_r[0]
    return (
        grad_wg.astype(jnp.bfloat16)[None],
        grad_wu.astype(jnp.bfloat16)[None],
        grad_down.astype(jnp.bfloat16)[None],
        d_out_weight,
        d_input,
        d_values,
        d_write,
        d_read,
        d_gate,
    )


def solution(mesh):
    return jax.shard_map(
        body,
        mesh=mesh,
        in_specs=(
            P("sp", None),
            P("sp", None),
            P("sp", None),
            P("sp", None),
            P("sp", None, "tp"),
            P("sp", None, "tp"),
            P("sp", "tp", None),
            P("tp", None),
            P("sp", "tp"),
            P("sp", "tp"),
            P("sp", "tp"),
            P("sp", "tp"),
            P("sp", "tp"),
            P("tp", "sp"),
            P("sp", "tp", None, None),
        ),
        out_specs=(
            P("sp", None, "tp"),
            P("sp", None, "tp"),
            P("sp", "tp", None),
            P("sp", "tp"),
            P("sp", "tp"),
            P("sp", "tp"),
            P("sp", "tp"),
            P("sp", "tp"),
            P("sp", "tp"),
        ),
        check_vma=False,
    )
```
